32 devices in a mesh: sp: 8 (over z, y), dp: 4 (over x, core).
Axes of the slice: x: 2, y: 2, z: 4, core: 2. Of those that a mesh axis runs over, the one named last changes fastest.
Arguments:
- hidden_in: bfloat16 [4, 1024, 2048], P('dp', 'sp'), may hold values from -6 to 6
- queries: bfloat16 [4, 1024, 1536], P('dp', 'sp'), may hold values from -64 to 64
- key_value_latent: bfloat16 [4, 1024, 512], P('dp', 'sp'), may hold values from -6 to 6
- keys_rope: bfloat16 [4, 1024, 32], P('dp', 'sp'), may hold values from -4 to 4
- latent_norm_gain: float32 [512], replicated, may hold values from 0.1 to 1.9
- latent_up_weight: bfloat16 [512, 2048], replicated, may hold values from -0.25 to 0.25
- attn_gain: float32 [1024], replicated, may hold values from 0.1 to 1.9
- out_proj: bfloat16 [1024, 2048], replicated, may hold values from -0.1875 to 0.1875
- norm1_gain: float32 [2048], replicated, may hold values from 0.1 to 1.9
- norm1_bias: float32 [2048], replicated, may hold values from -1.5 to 1.5
- expert_ids: int32 [4, 1024, 4], P('dp', 'sp'), may hold values from 0 to 31, all different within a row; in each aligned block of 128 rows (0 to 127, 128 to 255, ..., all dimensions but the last counted through in order) at most 24 rows name the same one
- route_weights: float32 [4, 1024, 4], P('dp', 'sp'), may hold values from 0.1 to 1
- gate_proj: bfloat16 [32, 2048, 512], P(('sp', 'dp')), may hold values from -0.125 to 0.125
- up_proj: bfloat16 [32, 2048, 512], P(('sp', 'dp')), may hold values from -0.125 to 0.125
- down_proj: bfloat16 [32, 512, 2048], P(('sp', 'dp')), may hold values from -0.25 to 0.25
- shared_gate: bfloat16 [2048, 512], replicated, may hold values from -0.125 to 0.125
- shared_up: bfloat16 [2048, 512], replicated, may hold values from -0.125 to 0.125
- shared_down: bfloat16 [512, 2048], replicated, may hold values from -0.25 to 0.25
- norm2_gain: float32 [2048], replicated, may hold values from 0.1 to 1.9
- norm2_bias: float32 [2048], replicated, may hold values from -1.5 to 1.5
Outputs:
- result: bfloat16 [4, 1024, 2048], P('dp', 'sp')
The draws below stay inside these ranges and needn't reach their ends.
Inputs may be any that keep to these rules, and one draw needn't show every extreme that they name: `expert_ids`: each row names 4 different experts. Among the rows of one device (aligned blocks of 128 rows), no expert is named more than 24 times, a bound that some block reaches.
All inputs are finite; a program needn't handle non-finite values.
Results may differ from the reference program's by a relative error of at most 0.01.
Values may be sent and summed in bfloat16 or wider, within the bound.
A program may use at most 128 MiB of HBM per device.

```python
import math
import jax
import jax.numpy as jnp
import numpy as np
from jax import lax

D = 2048
ATTENTION_HEADS = 16
PLAIN_HEAD_WIDTH = 64
QK_ROPE = 32
VALUE_HEAD_WIDTH = 64
LATENT_WIDTH = 512
D_EXPERT = 512
D_SHARED = 512
TOP_K = 4
TOK_DEV = 128
SEQUENCE_LENGTH = 1024
BATCH_SEQUENCES = 4
D_ATTN = 1024
EXPERTS = 32
CAP = 24


def rope_base(key):
    inner = jax.random.fold_in(key, 71)
    return jnp.clip(jax.random.normal(inner, (BATCH_SEQUENCES, SEQUENCE_LENGTH, QK_ROPE), jnp.float32), -4.0, 4.0)


def draw_keys_rope(key, part):
    return rope_base(key).astype(jnp.bfloat16)


def draw_queries(key, part):
    head_width = PLAIN_HEAD_WIDTH + QK_ROPE
    inner = jax.random.fold_in(key, 13)
    base = jnp.clip(jax.random.normal(inner, (BATCH_SEQUENCES, SEQUENCE_LENGTH, ATTENTION_HEADS, head_width), jnp.float32), -6.0, 6.0)
    return base.reshape(BATCH_SEQUENCES, SEQUENCE_LENGTH, ATTENTION_HEADS * head_width).astype(jnp.bfloat16)


def steps_of(stream_key, shape, cuts, low, largest):
    loudness, own = 1.0, jax.random.fold_in(stream_key, 6)
    for dim, blocks in cuts:
        steps = jnp.exp(jax.random.uniform(jax.random.fold_in(own, dim), (blocks,), jnp.float32, low / len(cuts), largest / len(cuts)))
        loudness = loudness * jnp.repeat(steps, shape[dim] // blocks).reshape([-1 if axis == dim else 1 for axis in range(len(shape))])
    return loudness


def routed_block(rng, own, number, rows, amount, top, bound, slope):
    sequence = jax.random.permutation(rng, amount)
    heavy_load, common = shares(amount, rows * top, bound, slope, True), shares(amount, rows * top, bound, slope, False)
    places = jnp.arange(amount)

    def named(tallies, offset_by):
        used = int((tallies > 0).sum())
        fixed = max(1, used // 4)
        moved = fixed + (places - fixed + offset_by * (used - fixed)) % max(1, amount - fixed)
        return jnp.zeros((amount,), jnp.int32).at[sequence[jnp.where(places < fixed, places, moved)]].set(jnp.asarray(tallies, jnp.int32))

    tallies = jnp.where(number % 4 == 0, named(heavy_load, number // 4), named(common, number - number // 4 - 1))
    mixed = jax.random.permutation(jax.random.fold_in(own, 3), amount)
    source_of, sink = mixed[0:amount // 2 * 2:2], mixed[1:amount // 2 * 2:2]
    slack = jnp.minimum(tallies[source_of] - 1, bound - tallies[sink]) // 2
    slack = jnp.where((source_of == sequence[0]) | (sink == sequence[0]) | (tallies[sink] == 0), 0, jnp.maximum(slack, 0))
    moved = jax.random.randint(jax.random.fold_in(own, 4), (amount // 2,), 0, 1 << 20) % (slack + 1)
    tallies = tallies.at[source_of].add(-moved).at[sink].add(moved)
    labels = jnp.searchsorted(jnp.cumsum(tallies), jnp.arange(rows * top), side="right").astype(jnp.int32)
    grid = labels.reshape(top, rows).T
    grid = grid[jax.random.permutation(jax.random.fold_in(own, 1), rows)]
    offset_by = jax.random.randint(jax.random.fold_in(own, 2), (rows, 1), 0, top)
    return jnp.take_along_axis(grid, (jnp.arange(top)[None, :] + offset_by) % top, axis=1)


def shares(number_of, total, limit, slope, full):
    portions = [(1 << 20) // math.isqrt(rank ** slope) + 1 for rank in range(1, number_of + 1)]
    largest = limit if full else min(limit, max(-(-total // number_of), total * portions[0] // sum(portions)))
    least = 1 if total - largest >= number_of - 1 else 0
    counts, surplus = [largest] + [least] * (number_of - 1), total - largest - least * (number_of - 1)
    while surplus > 0:
        candidates = [i for i in range(1, number_of) if counts[i] < largest] or [i for i in range(1, number_of) if counts[i] < limit]
        whole, budget = sum([portions[i] for i in candidates]), surplus
        for i in candidates:
            more = min(limit - counts[i], max(1, budget * portions[i] // whole), surplus)
            counts[i] = counts[i] + more
            surplus = surplus - more
    return np.array(counts)


def scatter_about(stream_key, dims, width, reach, shards=(), kind=jnp.bfloat16):
    values = width * jax.random.normal(stream_key, dims, jnp.float32)
    if shards:
        values = values * steps_of(stream_key, dims, shards, -0.22, 0.18)
    return jnp.clip(values, -reach, reach).astype(kind)


def setup_inputs(seed: int = 0) -> dict:
    splits = jax.random.split(jax.random.key(seed), 21)
    hidden_in = scatter_about(splits[0], (BATCH_SEQUENCES, SEQUENCE_LENGTH, D), 1.0, 6.0, ((0, 4), (1, 8)))
    queries = draw_queries(jax.random.fold_in(splits[20], 71), 0)
    key_value_latent = scatter_about(splits[2], (BATCH_SEQUENCES, SEQUENCE_LENGTH, LATENT_WIDTH), 1.0, 6.0, ((0, 4), (1, 8)))
    keys_rope = draw_keys_rope(jax.random.fold_in(splits[20], 71), 0)
    latent_norm_gain = jnp.clip(1.0 + 0.18 * jax.random.normal(splits[4], (LATENT_WIDTH,), jnp.float32), 0.1, 1.9)
    latent_up_weight = scatter_about(splits[5], (LATENT_WIDTH, ATTENTION_HEADS * (PLAIN_HEAD_WIDTH + VALUE_HEAD_WIDTH)), LATENT_WIDTH ** -0.5, 0.25)
    attn_gain = jnp.clip(1.0 + 0.18 * jax.random.normal(splits[6], (D_ATTN,), jnp.float32), 0.1, 1.9)
    out_proj = scatter_about(splits[7], (D_ATTN, D), D_ATTN ** -0.5, 0.1875)
    norm1_gain = jnp.clip(1.0 + 0.18 * jax.random.normal(splits[8], (D,), jnp.float32), 0.1, 1.9)
    norm1_bias = scatter_about(splits[9], (D,), 0.3, 1.5, (), jnp.float32)
    expert_ids_keys = jax.random.split(jax.random.fold_in(splits[10], 1), BATCH_SEQUENCES * SEQUENCE_LENGTH // TOK_DEV)
    expert_ids_turns = jax.random.permutation(jax.random.fold_in(splits[10], 3), BATCH_SEQUENCES * SEQUENCE_LENGTH // TOK_DEV)
    expert_ids = jax.vmap(lambda own, number: routed_block(jax.random.fold_in(splits[10], 2), own, number, TOK_DEV, EXPERTS, TOP_K, CAP, 2))(expert_ids_keys, expert_ids_turns).reshape((BATCH_SEQUENCES, SEQUENCE_LENGTH, TOP_K))
    route_weights = jnp.clip(0.1 + 0.9 * jax.random.uniform(splits[11], (BATCH_SEQUENCES, SEQUENCE_LENGTH, TOP_K), jnp.float32) ** steps_of(splits[11], (BATCH_SEQUENCES, SEQUENCE_LENGTH, TOP_K), ((0, 4), (1, 8)), -0.2, 0.2), 0.1, 1.0)
    gate_proj = scatter_about(splits[12], (EXPERTS, D, D_EXPERT), D ** -0.5, 0.125, ((0, 32),))
    up_proj = scatter_about(splits[13], (EXPERTS, D, D_EXPERT), D ** -0.5, 0.125, ((0, 32),))
    down_proj = scatter_about(splits[14], (EXPERTS, D_EXPERT, D), D_EXPERT ** -0.5, 0.25, ((0, 32),))
    shared_gate = scatter_about(splits[15], (D, D_SHARED), D ** -0.5, 0.125)
    shared_up = scatter_about(splits[16], (D, D_SHARED), D ** -0.5, 0.125)
    shared_down = scatter_about(splits[17], (D_SHARED, D), D_SHARED ** -0.5, 0.25)
    norm2_gain = jnp.clip(1.0 + 0.18 * jax.random.normal(splits[18], (D,), jnp.float32), 0.1, 1.9)
    norm2_bias = scatter_about(splits[19], (D,), 0.3, 1.5, (), jnp.float32)
    return {"hidden_in": hidden_in, "queries": queries, "key_value_latent": key_value_latent, "keys_rope": keys_rope, "latent_norm_gain": latent_norm_gain, "latent_up_weight": latent_up_weight, "attn_gain": attn_gain, "out_proj": out_proj, "norm1_gain": norm1_gain, "norm1_bias": norm1_bias, "expert_ids": expert_ids, "route_weights": route_weights, "gate_proj": gate_proj, "up_proj": up_proj, "down_proj": down_proj, "shared_gate": shared_gate, "shared_up": shared_up, "shared_down": shared_down, "norm2_gain": norm2_gain, "norm2_bias": norm2_bias}


ALPHA = 2.0 ** 0.25
ROUTED = 2.5
THETA = 10000.0

def rms_scaled(values, scaling):
    widened = values.astype(jnp.float32)
    return widened * lax.rsqrt(lax.optimization_barrier(jnp.mean(widened * widened, axis=-1, keepdims=True)) + 1e-06) * scaling

def layer_norm(values, scaling, bias_add):
    centre = values - lax.optimization_barrier(jnp.mean(values, axis=-1, keepdims=True))
    spread = lax.optimization_barrier(jnp.mean(centre * centre, axis=-1, keepdims=True))
    return centre * lax.rsqrt(spread + 1e-05) * scaling + bias_add

def rotation_tables(positions, rot_width):
    frequency = THETA ** (-jnp.arange(0, rot_width, 2, dtype=jnp.float32) / rot_width)
    angles = positions.astype(jnp.float32)[:, None] * frequency[None, :]
    return (jnp.cos(angles), jnp.sin(angles))

def turn(values, cosine_table, sine_table):
    half_width = values.shape[-1] // 2
    first_half = values[..., :half_width]
    second_half = values[..., half_width:]
    return jnp.concatenate([first_half * cosine_table - second_half * sine_table, second_half * cosine_table + first_half * sine_table], axis=-1)

def attend(query, key_full, values):
    length = query.shape[0]
    span_rows = 512 if length % 512 == 0 else length
    block_count = length // span_rows
    blocks = query.reshape(block_count, span_rows, query.shape[1])
    key_pos = jnp.arange(length, dtype=jnp.int32)
    factor = 1.0 / math.sqrt(query.shape[1])

    def one_block(inputs):
        block_index, query_rows = inputs
        scores = jnp.dot(query_rows, key_full.T, preferred_element_type=jnp.float32) * factor
        query_pos = block_index * span_rows + jnp.arange(span_rows, dtype=jnp.int32)
        scores = jnp.where(key_pos[None, :] <= query_pos[:, None], scores, -jnp.inf)
        row_max = lax.optimization_barrier(jnp.max(scores, axis=-1, keepdims=True))
        weights = jnp.exp(scores - row_max)
        weights = (weights / lax.optimization_barrier(jnp.sum(weights, axis=-1, keepdims=True))).astype(jnp.bfloat16)
        return jnp.dot(weights, values, preferred_element_type=jnp.float32).astype(jnp.bfloat16)
    attended = lax.map(one_block, (jnp.arange(block_count, dtype=jnp.int32), blocks))
    return attended.reshape(length, values.shape[1])

def swiglu_rows(rows, gate_mat, up_mat, down_mat):
    gated = jnp.dot(rows, gate_mat, preferred_element_type=jnp.float32)
    lifted = jnp.dot(rows, up_mat, preferred_element_type=jnp.float32)
    inner = (jax.nn.silu(gated) * lifted).astype(jnp.bfloat16)
    return jnp.dot(inner, down_mat, preferred_element_type=jnp.float32)

def mixer_sequence(hidden_seq, query_seq, latent_seq, rope_seq, latent_norm_gain, latent_up_weight, attn_gain, out_proj, norm1_gain, norm1_bias):
    length = hidden_seq.shape[0]
    normed = rms_scaled(latent_seq, latent_norm_gain).astype(jnp.bfloat16)
    keys_values = jnp.dot(normed, latent_up_weight, preferred_element_type=jnp.float32).astype(jnp.bfloat16)
    keys_values = keys_values.reshape(length, ATTENTION_HEADS, PLAIN_HEAD_WIDTH + VALUE_HEAD_WIDTH)
    cosine_table, sine_table = rotation_tables(jnp.arange(length, dtype=jnp.int32), QK_ROPE)
    keys_turned = turn(rope_seq.astype(jnp.float32), cosine_table, sine_table).astype(jnp.bfloat16)
    query_heads = query_seq.reshape(length, ATTENTION_HEADS, PLAIN_HEAD_WIDTH + QK_ROPE)
    query_turned = turn(query_heads[..., PLAIN_HEAD_WIDTH:].astype(jnp.float32), cosine_table[:, None, :], sine_table[:, None, :]).astype(jnp.bfloat16)
    query_full = jnp.concatenate([query_heads[..., :PLAIN_HEAD_WIDTH], query_turned], axis=-1)
    key_full = jnp.concatenate([keys_values[..., :PLAIN_HEAD_WIDTH], jnp.broadcast_to(keys_turned[:, None, :], (length, ATTENTION_HEADS, QK_ROPE))], axis=-1)
    values_heads = keys_values[..., PLAIN_HEAD_WIDTH:]
    by_head = lax.map(lambda inputs: attend(inputs[0], inputs[1], inputs[2]), (jnp.moveaxis(query_full, 1, 0), jnp.moveaxis(key_full, 1, 0), jnp.moveaxis(values_heads, 1, 0)))
    attended = jnp.moveaxis(by_head, 0, 1).reshape(length, ATTENTION_HEADS * VALUE_HEAD_WIDTH)
    attn_normed = rms_scaled(attended, attn_gain).astype(jnp.bfloat16)
    mixed = jnp.dot(attn_normed, out_proj, preferred_element_type=jnp.float32)
    return layer_norm(ALPHA * hidden_seq.astype(jnp.float32) + mixed, norm1_gain, norm1_bias).astype(jnp.bfloat16)

def reference(hidden_in, queries, key_value_latent, keys_rope, latent_norm_gain, latent_up_weight, attn_gain, out_proj, norm1_gain, norm1_bias, expert_ids, route_weights, gate_proj, up_proj, down_proj, shared_gate, shared_up, shared_down, norm2_gain, norm2_bias):
    batch_count = hidden_in.shape[0]
    length = hidden_in.shape[1]
    firsts = [mixer_sequence(hidden_in[member], queries[member], key_value_latent[member], keys_rope[member], latent_norm_gain, latent_up_weight, attn_gain, out_proj, norm1_gain, norm1_bias) for member in range(batch_count)]
    first = jnp.concatenate(firsts, axis=0)
    total = first.shape[0]
    blocks = total // TOK_DEV
    entries = expert_ids.reshape(blocks, TOK_DEV * TOP_K).astype(jnp.int32)
    onehot = (entries[:, :, None] == jnp.arange(EXPERTS, dtype=jnp.int32)[None, None, :]).astype(jnp.int32)
    earlier = jnp.cumsum(onehot, axis=1).astype(jnp.int32) - onehot
    slots = lax.optimization_barrier(jnp.sum(earlier * onehot, axis=-1)).astype(jnp.int32)
    block_ids = jnp.arange(blocks, dtype=jnp.int32)[:, None]
    places = (entries * (blocks * CAP) + block_ids * CAP + slots).reshape(-1).astype(jnp.int32)
    owners = (jnp.arange(total * TOP_K, dtype=jnp.int32) // TOP_K).astype(jnp.int32)
    table = jnp.full((EXPERTS * blocks * CAP,), total, jnp.int32).at[places].set(owners)
    padded = jnp.concatenate([first, jnp.zeros((1, D), jnp.bfloat16)], axis=0)

    def expert_block(inputs):
        gate_mat, up_mat, down_mat, picks = inputs
        return swiglu_rows(padded[picks], gate_mat, up_mat, down_mat).astype(jnp.bfloat16)
    expert_out = lax.map(expert_block, (gate_proj, up_proj, down_proj, table.reshape(EXPERTS, blocks * CAP)))
    gathered = expert_out.reshape(EXPERTS * blocks * CAP, D)[places].reshape(total, TOP_K, D)
    weights = route_weights.reshape(total, TOP_K).astype(jnp.float32)
    gates = weights / lax.optimization_barrier(jnp.sum(weights, axis=-1, keepdims=True)) * ROUTED
    routed = jnp.zeros((total, D), jnp.float32)
    for column in range(TOP_K):
        routed = routed + gates[:, column:column + 1] * gathered[:, column].astype(jnp.float32)
    feed = routed + swiglu_rows(first, shared_gate, shared_up, shared_down)
    result = layer_norm(ALPHA * first.astype(jnp.float32) + feed, norm2_gain, norm2_bias).astype(jnp.bfloat16)
    return result.reshape(batch_count, length, D)
```

```python
import functools
import math

import jax
import jax.numpy as jnp
from jax import lax
from jax.experimental import pallas as pl
from jax.experimental.pallas import tpu as pltpu
from jax.sharding import PartitionSpec as P

D = 2048
ATTENTION_HEADS = 16
PLAIN_HEAD_WIDTH = 64
QK_ROPE = 32
VALUE_HEAD_WIDTH = 64
TOP_K = 4


ALPHA = 2.0**0.25
ROUTED = 2.5
THETA = 10000.0


def rms_scaled(values, scaling):
    widened = values.astype(jnp.float32)
    return (
        widened * lax.rsqrt(jnp.mean(widened * widened, axis=-1, keepdims=True) + 1e-06) * scaling
    )


def layer_norm(values, scaling, bias_add):
    centre = values - jnp.mean(values, axis=-1, keepdims=True)
    spread = jnp.mean(centre * centre, axis=-1, keepdims=True)
    return centre * lax.rsqrt(spread + 1e-05) * scaling + bias_add


def rotation_tables(positions, rot_width):
    frequency = THETA ** (-jnp.arange(0, rot_width, 2, dtype=jnp.float32) / rot_width)
    angles = positions.astype(jnp.float32)[:, None] * frequency[None, :]
    return (jnp.cos(angles), jnp.sin(angles))


def turn(values, cosine_table, sine_table):
    half_width = values.shape[-1] // 2
    first_half = values[..., :half_width]
    second_half = values[..., half_width:]
    return jnp.concatenate(
        [
            first_half * cosine_table - second_half * sine_table,
            second_half * cosine_table + first_half * sine_table,
        ],
        axis=-1,
    )


MESH = pl.DeviceIdType.MESH
LANES = 128


def inner_of(count):
    return count // 4 if count % 4 == 0 else 1


def gather_kernel(count, x_ref, out_ref, own_sem, send_sem, recv_sem):
    inner = inner_of(count)
    outer = count // inner
    me = lax.axis_index("sp")
    far, near = me // inner, me % inner
    far_peers = [((far + step) % outer) * inner + near for step in range(1, outer)]
    near_peers = [far * inner + (near + step) % inner for step in range(1, inner)]

    barrier = pltpu.get_barrier_semaphore()
    for peer in far_peers + near_peers:
        pl.semaphore_signal(barrier, inc=1, device_id={"sp": peer}, device_id_type=MESH)
    pl.semaphore_wait(barrier, len(far_peers) + len(near_peers))

    started = []

    def send(source, owner, peer):
        copy = pltpu.make_async_remote_copy(
            src_ref=source,
            dst_ref=out_ref.at[owner],
            send_sem=send_sem.at[len(started)],
            recv_sem=recv_sem.at[owner],
            device_id={"sp": peer},
            device_id_type=MESH,
        )
        copy.start()
        started.append(copy)

    def arrive(owner):
        pltpu.make_async_remote_copy(
            src_ref=x_ref,
            dst_ref=out_ref.at[owner],
            send_sem=send_sem.at[0],
            recv_sem=recv_sem.at[owner],
            device_id={"sp": (me + 1) % count},
            device_id_type=MESH,
        ).wait_recv()

    for peer in far_peers + near_peers:
        send(x_ref, me, peer)
    own = pltpu.make_async_copy(x_ref, out_ref.at[me], own_sem)
    own.start()
    for step in range(1, outer):
        owner = ((far + outer - step) % outer) * inner + near
        arrive(owner)
        for peer in near_peers:
            send(out_ref.at[owner], owner, peer)
    for other in range(1, inner):
        for step in range(outer):
            arrive(((far + outer - step) % outer) * inner + (near + inner - other) % inner)
    own.wait()
    for copy in started:
        copy.wait_send()


def gather_rows(block):
    count = lax.axis_size("sp")
    inner = inner_of(count)
    outer = count // inner
    sends = (outer - 1) + (inner - 1) * outer
    rows, width = block.shape
    return pl.pallas_call(
        functools.partial(gather_kernel, count),
        out_shape=jax.ShapeDtypeStruct((count, rows, width), block.dtype),
        in_specs=[pl.BlockSpec(memory_space=pltpu.VMEM)],
        out_specs=pl.BlockSpec(memory_space=pltpu.VMEM),
        scratch_shapes=[
            pltpu.SemaphoreType.DMA,
            pltpu.SemaphoreType.DMA((sends,)),
            pltpu.SemaphoreType.DMA((count,)),
        ],
        compiler_params=pltpu.CompilerParams(collective_id=0, has_side_effects=True),
    )(block).reshape(count * rows, width)


PAIR = 2


def attend_kernel(offset_ref, query_ref, whole_ref, up_ref, out_ref):
    rows = query_ref.shape[2]
    latent_width = up_ref.shape[0]
    length = whole_ref.shape[0]
    head_width = PLAIN_HEAD_WIDTH + VALUE_HEAD_WIDTH
    factor = math.log2(math.e) / math.sqrt(PLAIN_HEAD_WIDTH + QK_ROPE)
    latents = whole_ref[:, :latent_width]
    turned = whole_ref[:, latent_width:]
    pairs = jnp.dot(latents, up_ref[...], preferred_element_type=jnp.float32).astype(jnp.bfloat16)
    query_pos = offset_ref[0] + lax.broadcasted_iota(jnp.int32, (rows, length), 0)
    visible = lax.broadcasted_iota(jnp.int32, (rows, length), 1) <= query_pos
    outs = []
    for head in range(PAIR):
        block = pairs[:, head * head_width : (head + 1) * head_width]
        keys = jnp.concatenate([block, turned], axis=1)
        scores = lax.dot_general(
            query_ref[0, head], keys, (((1,), (1,)), ((), ())), preferred_element_type=jnp.float32
        )
        scores = jnp.where(visible, scores, -jnp.inf)
        row_max = jnp.max(scores, axis=-1, keepdims=True)
        weights = jnp.exp2((scores - row_max) * factor)
        total = jnp.sum(weights, axis=-1, keepdims=True)
        mixed = jnp.dot(weights.astype(jnp.bfloat16), block, preferred_element_type=jnp.float32)
        outs.append((mixed / total)[:, PLAIN_HEAD_WIDTH:])
    out_ref[...] = jnp.concatenate(outs, axis=1).astype(out_ref.dtype)


def attend(query_full, whole, up_weight, offset):
    rows = query_full.shape[1]
    steps = ATTENTION_HEADS // PAIR
    span = PAIR * (PLAIN_HEAD_WIDTH + VALUE_HEAD_WIDTH)
    width = query_full.shape[2]
    return pl.pallas_call(
        attend_kernel,
        grid=(steps,),
        out_shape=jax.ShapeDtypeStruct((rows, ATTENTION_HEADS * VALUE_HEAD_WIDTH), jnp.bfloat16),
        in_specs=[
            pl.BlockSpec(memory_space=pltpu.SMEM),
            pl.BlockSpec((1, PAIR, rows, width), lambda step: (step, 0, 0, 0)),
            pl.BlockSpec(whole.shape, lambda step: (0, 0)),
            pl.BlockSpec((up_weight.shape[0], span), lambda step: (0, step)),
        ],
        out_specs=pl.BlockSpec((rows, PAIR * VALUE_HEAD_WIDTH), lambda step: (0, step)),
    )(offset, query_full.reshape(steps, PAIR, rows, width), whole, up_weight)


def swiglu_rows(rows, gate_mat, up_mat, down_mat):
    gated = jnp.dot(rows, gate_mat, preferred_element_type=jnp.float32)
    lifted = jnp.dot(rows, up_mat, preferred_element_type=jnp.float32)
    inner = (jax.nn.silu(gated) * lifted).astype(jnp.bfloat16)
    return jnp.dot(inner, down_mat, preferred_element_type=jnp.float32)


def per_device(
    hidden_in,
    queries,
    key_value_latent,
    keys_rope,
    latent_norm_gain,
    latent_up_weight,
    attn_gain,
    out_proj,
    norm1_gain,
    norm1_bias,
    expert_ids,
    route_weights,
    gate_proj,
    up_proj,
    down_proj,
    shared_gate,
    shared_up,
    shared_down,
    norm2_gain,
    norm2_bias,
):
    tok_rows = hidden_in.shape[1]
    normed = rms_scaled(key_value_latent[0], latent_norm_gain).astype(jnp.bfloat16)
    start = lax.axis_index("sp") * tok_rows
    local_pos = start + jnp.arange(tok_rows, dtype=jnp.int32)
    cos_local, sin_local = rotation_tables(local_pos, QK_ROPE)
    keys_turned = turn(keys_rope[0].astype(jnp.float32), cos_local, sin_local).astype(jnp.bfloat16)
    whole = gather_rows(
        jnp.concatenate([normed, jnp.pad(keys_turned, ((0, 0), (0, LANES - QK_ROPE)))], axis=1)
    )
    query_heads = queries[0].reshape(tok_rows, ATTENTION_HEADS, PLAIN_HEAD_WIDTH + QK_ROPE)
    query_turned = turn(
        query_heads[..., PLAIN_HEAD_WIDTH:].astype(jnp.float32),
        cos_local[:, None, :],
        sin_local[:, None, :],
    ).astype(jnp.bfloat16)
    query_full = jnp.concatenate(
        [
            query_heads[..., :PLAIN_HEAD_WIDTH],
            jnp.zeros((tok_rows, ATTENTION_HEADS, VALUE_HEAD_WIDTH), jnp.bfloat16),
            query_turned,
            jnp.zeros((tok_rows, ATTENTION_HEADS, LANES - QK_ROPE), jnp.bfloat16),
        ],
        axis=-1,
    )
    attended = attend(
        jnp.moveaxis(query_full, 1, 0), whole, latent_up_weight, start.reshape(1).astype(jnp.int32)
    )
    attn_normed = rms_scaled(attended, attn_gain).astype(jnp.bfloat16)
    mixed = jnp.dot(attn_normed, out_proj, preferred_element_type=jnp.float32)
    first = layer_norm(
        ALPHA * hidden_in[0].astype(jnp.float32) + mixed, norm1_gain, norm1_bias
    ).astype(jnp.bfloat16)
    group = lax.axis_size("sp") * lax.axis_size("dp")
    capacity = (tok_rows * TOP_K * 3 + 2 * group - 1) // (2 * group)
    entries = expert_ids[0].reshape(-1)
    onehot = (entries[:, None] == jnp.arange(group, dtype=jnp.int32)[None, :]).astype(jnp.int32)
    earlier = jnp.cumsum(onehot, axis=0) - onehot
    slots = jnp.sum(earlier * onehot, axis=-1)
    places = (entries * capacity + slots).reshape(tok_rows, TOP_K)
    slot_ids = jnp.arange(group * capacity, dtype=jnp.int32)
    dispatch = jnp.any(places[None, :, :] == slot_ids[:, None, None], axis=-1).astype(jnp.bfloat16)
    outbound = jnp.dot(dispatch, first, preferred_element_type=jnp.float32).astype(jnp.bfloat16)
    arrived = lax.all_to_all(
        outbound.reshape(group, capacity, D), ("sp", "dp"), split_axis=0, concat_axis=0, tiled=True
    )
    flat_rows = arrived.reshape(group * capacity, D)
    produced = (
        swiglu_rows(flat_rows, gate_proj[0], up_proj[0], down_proj[0])
        .astype(jnp.bfloat16)
        .reshape(group, capacity, D)
    )
    returned = lax.all_to_all(produced, ("sp", "dp"), split_axis=0, concat_axis=0, tiled=True)
    returned_flat = returned.reshape(group * capacity, D)
    weights = route_weights[0]
    gates = weights / jnp.sum(weights, axis=-1, keepdims=True) * ROUTED
    routed = jnp.zeros((tok_rows, D), jnp.float32)
    for column in range(TOP_K):
        picker = (places[:, column : column + 1] == slot_ids[None, :]).astype(jnp.bfloat16)
        picked = jnp.dot(picker, returned_flat, preferred_element_type=jnp.float32)
        routed = routed + gates[:, column : column + 1] * picked
    feed = routed + swiglu_rows(first, shared_gate, shared_up, shared_down)
    result = layer_norm(ALPHA * first.astype(jnp.float32) + feed, norm2_gain, norm2_bias).astype(
        jnp.bfloat16
    )
    return result.reshape(1, tok_rows, D)


def solution(mesh):
    in_specs = (
        P("dp", "sp", None),
        P("dp", "sp", None),
        P("dp", "sp", None),
        P("dp", "sp", None),
        P(),
        P(),
        P(),
        P(),
        P(),
        P(),
        P("dp", "sp", None),
        P("dp", "sp", None),
        P(("sp", "dp"), None, None),
        P(("sp", "dp"), None, None),
        P(("sp", "dp"), None, None),
        P(),
        P(),
        P(),
        P(),
        P(),
    )
    out_specs = P("dp", "sp", None)
    return jax.shard_map(
        per_device, mesh=mesh, in_specs=in_specs, out_specs=out_specs, check_vma=False
    )
```

```python
import functools
import math

import jax
import jax.numpy as jnp
from jax import lax
from jax.experimental import pallas as pl
from jax.experimental.pallas import tpu as pltpu
from jax.sharding import PartitionSpec as P

D = 2048
ATTENTION_HEADS = 16
PLAIN_HEAD_WIDTH = 64
QK_ROPE = 32
VALUE_HEAD_WIDTH = 64
TOP_K = 4


ALPHA = 2.0**0.25
ROUTED = 2.5
THETA = 10000.0


def rms_scaled(values, scaling):
    widened = values.astype(jnp.float32)
    return (
        widened * lax.rsqrt(jnp.mean(widened * widened, axis=-1, keepdims=True) + 1e-06) * scaling
    )


def layer_norm(values, scaling, bias_add):
    centre = values - jnp.mean(values, axis=-1, keepdims=True)
    spread = jnp.mean(centre * centre, axis=-1, keepdims=True)
    return centre * lax.rsqrt(spread + 1e-05) * scaling + bias_add


def rotation_tables(positions, rot_width):
    frequency = THETA ** (-jnp.arange(0, rot_width, 2, dtype=jnp.float32) / rot_width)
    angles = positions.astype(jnp.float32)[:, None] * frequency[None, :]
    return (jnp.cos(angles), jnp.sin(angles))


def turn(values, cosine_table, sine_table):
    half_width = values.shape[-1] // 2
    first_half = values[..., :half_width]
    second_half = values[..., half_width:]
    return jnp.concatenate(
        [
            first_half * cosine_table - second_half * sine_table,
            second_half * cosine_table + first_half * sine_table,
        ],
        axis=-1,
    )


MESH = pl.DeviceIdType.MESH
LANES = 128


def inner_of(count):
    return count // 4 if count % 4 == 0 else 1


def gather_kernel(count, x_ref, out_ref, own_sem, send_sem, recv_sem):
    inner = inner_of(count)
    outer = count // inner
    me = lax.axis_index("sp")
    far, near = me // inner, me % inner
    far_peers = [((far + step) % outer) * inner + near for step in range(1, outer)]
    near_peers = [far * inner + (near + step) % inner for step in range(1, inner)]

    barrier = pltpu.get_barrier_semaphore()
    for peer in far_peers + near_peers:
        pl.semaphore_signal(barrier, inc=1, device_id={"sp": peer}, device_id_type=MESH)
    pl.semaphore_wait(barrier, len(far_peers) + len(near_peers))

    started = []

    def send(source, owner, peer):
        copy = pltpu.make_async_remote_copy(
            src_ref=source,
            dst_ref=out_ref.at[owner],
            send_sem=send_sem.at[len(started)],
            recv_sem=recv_sem.at[owner],
            device_id={"sp": peer},
            device_id_type=MESH,
        )
        copy.start()
        started.append(copy)

    def arrive(owner):
        pltpu.make_async_remote_copy(
            src_ref=x_ref,
            dst_ref=out_ref.at[owner],
            send_sem=send_sem.at[0],
            recv_sem=recv_sem.at[owner],
            device_id={"sp": (me + 1) % count},
            device_id_type=MESH,
        ).wait_recv()

    for peer in far_peers + near_peers:
        send(x_ref, me, peer)
    own = pltpu.make_async_copy(x_ref, out_ref.at[me], own_sem)
    own.start()
    for step in range(1, outer):
        owner = ((far + outer - step) % outer) * inner + near
        arrive(owner)
        for peer in near_peers:
            send(out_ref.at[owner], owner, peer)
    for other in range(1, inner):
        for step in range(outer):
            arrive(((far + outer - step) % outer) * inner + (near + inner - other) % inner)
    own.wait()
    for copy in started:
        copy.wait_send()


def gather_rows(block):
    count = lax.axis_size("sp")
    inner = inner_of(count)
    outer = count // inner
    sends = (outer - 1) + (inner - 1) * outer
    rows, width = block.shape
    return pl.pallas_call(
        functools.partial(gather_kernel, count),
        out_shape=jax.ShapeDtypeStruct((count, rows, width), block.dtype),
        in_specs=[pl.BlockSpec(memory_space=pltpu.VMEM)],
        out_specs=pl.BlockSpec(memory_space=pltpu.VMEM),
        scratch_shapes=[
            pltpu.SemaphoreType.DMA,
            pltpu.SemaphoreType.DMA((sends,)),
            pltpu.SemaphoreType.DMA((count,)),
        ],
        compiler_params=pltpu.CompilerParams(collective_id=0, has_side_effects=True),
    )(block).reshape(count * rows, width)


PAIR = 2


def attend_kernel(offset_ref, query_ref, whole_ref, up_ref, out_ref):
    rows = query_ref.shape[2]
    latent_width = up_ref.shape[0]
    length = whole_ref.shape[0]
    head_width = PLAIN_HEAD_WIDTH + VALUE_HEAD_WIDTH
    factor = math.log2(math.e) / math.sqrt(PLAIN_HEAD_WIDTH + QK_ROPE)
    latents = whole_ref[:, :latent_width]
    turned = whole_ref[:, latent_width:]
    pairs = jnp.dot(latents, up_ref[...], preferred_element_type=jnp.float32).astype(jnp.bfloat16)
    query_pos = offset_ref[0] + lax.broadcasted_iota(jnp.int32, (rows, length), 0)
    visible = lax.broadcasted_iota(jnp.int32, (rows, length), 1) <= query_pos
    outs = []
    for head in range(PAIR):
        block = pairs[:, head * head_width : (head + 1) * head_width]
        keys = jnp.concatenate([block, turned], axis=1)
        scores = lax.dot_general(
            query_ref[0, head], keys, (((1,), (1,)), ((), ())), preferred_element_type=jnp.float32
        )
        scores = jnp.where(visible, scores, -jnp.inf)
        row_max = jnp.max(scores, axis=-1, keepdims=True)
        weights = jnp.exp2((scores - row_max) * factor)
        total = jnp.sum(weights, axis=-1, keepdims=True)
        mixed = jnp.dot(weights.astype(jnp.bfloat16), block, preferred_element_type=jnp.float32)
        outs.append((mixed / total)[:, PLAIN_HEAD_WIDTH:])
    out_ref[...] = jnp.concatenate(outs, axis=1).astype(out_ref.dtype)


def attend(query_full, whole, up_weight, offset):
    rows = query_full.shape[1]
    steps = ATTENTION_HEADS // PAIR
    span = PAIR * (PLAIN_HEAD_WIDTH + VALUE_HEAD_WIDTH)
    width = query_full.shape[2]
    return pl.pallas_call(
        attend_kernel,
        grid=(steps,),
        out_shape=jax.ShapeDtypeStruct((rows, ATTENTION_HEADS * VALUE_HEAD_WIDTH), jnp.bfloat16),
        in_specs=[
            pl.BlockSpec(memory_space=pltpu.SMEM),
            pl.BlockSpec((1, PAIR, rows, width), lambda step: (step, 0, 0, 0)),
            pl.BlockSpec(whole.shape, lambda step: (0, 0)),
            pl.BlockSpec((up_weight.shape[0], span), lambda step: (0, step)),
        ],
        out_specs=pl.BlockSpec((rows, PAIR * VALUE_HEAD_WIDTH), lambda step: (0, step)),
    )(offset, query_full.reshape(steps, PAIR, rows, width), whole, up_weight)


def dispatch_kernel(
    first_ref, pick_ref, out_ref, held, outgoing,
    line_send, line_recv, send_sem, recv_sem, own_sem,
):
    count, ways = lax.axis_size("sp"), lax.axis_size("dp")
    inner = inner_of(count)
    outer = count // inner
    plane = inner * ways
    me = lax.axis_index("sp")
    far, near = me // inner, me % inner
    place = near * ways + lax.axis_index("dp")
    up_ok, down_ok = far < outer - 1, far > 0
    up = {"sp": jnp.minimum(far + 1, outer - 1) * inner + near}
    down = {"sp": jnp.maximum(far - 1, 0) * inner + near}

    def peer_of(step):
        peer = (place + step) % plane
        return peer, {"sp": far * inner + peer // ways, "dp": peer % ways}

    barrier = pltpu.get_barrier_semaphore()

    def greet(target):
        pl.semaphore_signal(barrier, inc=1, device_id=target, device_id_type=MESH)

    for step in range(1, outer):
        greet({"sp": ((far + step) % outer) * inner + near})

    @pl.loop(1, plane)
    def _(step):
        greet(peer_of(step)[1])

    pl.semaphore_wait(barrier, outer + plane - 2)

    def along(source, owner, side):
        return pltpu.make_async_remote_copy(
            src_ref=source,
            dst_ref=held.at[owner],
            send_sem=line_send.at[side, owner],
            recv_sem=line_recv.at[owner],
            device_id=(up, down)[side],
            device_id_type=MESH,
        )

    def across(owner, step):
        peer, target = peer_of(step)
        return pltpu.make_async_remote_copy(
            src_ref=outgoing.at[owner, peer],
            dst_ref=out_ref.at[owner, place],
            send_sem=send_sem.at[owner, peer],
            recv_sem=recv_sem.at[owner, place],
            device_id=target,
            device_id_type=MESH,
        )

    def own_copy(owner):
        return pltpu.make_async_copy(
            outgoing.at[owner, place], out_ref.at[owner, place], own_sem.at[owner]
        )

    def spread(block, owner):
        rows = jnp.dot(pick_ref[owner], block, preferred_element_type=jnp.float32)
        outgoing[owner] = rows.reshape(outgoing.shape[1:]).astype(outgoing.dtype)

        @pl.loop(1, plane)
        def _(step):
            across(owner, step).start()

        own_copy(owner).start()

    pl.when(up_ok)(lambda: along(first_ref, far, 0).start())
    pl.when(down_ok)(lambda: along(first_ref, far, 1).start())
    spread(first_ref[...], far)
    for step in range(1, outer):
        @pl.when(far >= step)
        def _():
            owner = far - step
            along(first_ref, owner, 0).wait_recv()
            pl.when(up_ok)(lambda: along(held.at[owner], owner, 0).start())
            spread(held[owner], owner)

        @pl.when(far + step < outer)
        def _():
            owner = far + step
            along(first_ref, owner, 1).wait_recv()
            pl.when(down_ok)(lambda: along(held.at[owner], owner, 1).start())
            spread(held[owner], owner)

    for owner in range(outer):
        @pl.when(up_ok & (far >= owner))
        def _():
            along(first_ref, owner, 0).wait_send()

        @pl.when(down_ok & (far <= owner))
        def _():
            along(first_ref, owner, 1).wait_send()

        own_copy(owner).wait()

        @pl.loop(1, plane)
        def _(step):
            across(owner, step).wait_send()
            peer, target = peer_of(step)
            pltpu.make_async_remote_copy(
                src_ref=outgoing.at[owner, peer],
                dst_ref=out_ref.at[owner, peer],
                send_sem=send_sem.at[owner, peer],
                recv_sem=recv_sem.at[owner, peer],
                device_id=target,
                device_id_type=MESH,
            ).wait_recv()


def dispatch_rows(first, picks, slots):
    count, ways = lax.axis_size("sp"), lax.axis_size("dp")
    inner = inner_of(count)
    outer = count // inner
    plane = inner * ways
    shape = (outer, plane, slots, first.shape[1])
    return pl.pallas_call(
        dispatch_kernel,
        out_shape=jax.ShapeDtypeStruct(shape, first.dtype),
        in_specs=[pl.BlockSpec(memory_space=pltpu.VMEM)] * 2,
        out_specs=pl.BlockSpec(memory_space=pltpu.VMEM),
        scratch_shapes=[
            pltpu.VMEM((outer,) + first.shape, first.dtype),
            pltpu.VMEM(shape, first.dtype),
            pltpu.SemaphoreType.DMA((2, outer)),
            pltpu.SemaphoreType.DMA((outer,)),
            pltpu.SemaphoreType.DMA((outer, plane)),
            pltpu.SemaphoreType.DMA((outer, plane)),
            pltpu.SemaphoreType.DMA((outer,)),
        ],
        compiler_params=pltpu.CompilerParams(
            collective_id=1, has_side_effects=True, vmem_limit_bytes=40 * 2**20
        ),
    )(first, picks)


def swiglu_rows(rows, gate_mat, up_mat, down_mat):
    gated = jnp.dot(rows, gate_mat, preferred_element_type=jnp.float32)
    lifted = jnp.dot(rows, up_mat, preferred_element_type=jnp.float32)
    inner = (jax.nn.silu(gated) * lifted).astype(jnp.bfloat16)
    return jnp.dot(inner, down_mat, preferred_element_type=jnp.float32)


def per_device(
    hidden_in,
    queries,
    key_value_latent,
    keys_rope,
    latent_norm_gain,
    latent_up_weight,
    attn_gain,
    out_proj,
    norm1_gain,
    norm1_bias,
    expert_ids,
    route_weights,
    gate_proj,
    up_proj,
    down_proj,
    shared_gate,
    shared_up,
    shared_down,
    norm2_gain,
    norm2_bias,
):
    tok_rows = hidden_in.shape[1]
    normed = rms_scaled(key_value_latent[0], latent_norm_gain).astype(jnp.bfloat16)
    start = lax.axis_index("sp") * tok_rows
    local_pos = start + jnp.arange(tok_rows, dtype=jnp.int32)
    cos_local, sin_local = rotation_tables(local_pos, QK_ROPE)
    keys_turned = turn(keys_rope[0].astype(jnp.float32), cos_local, sin_local).astype(jnp.bfloat16)
    group = lax.axis_size("sp") * lax.axis_size("dp")
    capacity = (tok_rows * TOP_K * 3 + 2 * group - 1) // (2 * group)
    entries = expert_ids[0].reshape(-1)
    onehot = (entries[:, None] == jnp.arange(group, dtype=jnp.int32)[None, :]).astype(jnp.int32)
    earlier = jnp.cumsum(onehot, axis=0) - onehot
    slots = jnp.sum(earlier * onehot, axis=-1)
    places = (entries * capacity + slots).reshape(tok_rows, TOP_K)
    tags = jnp.concatenate([expert_ids[0], slots.reshape(tok_rows, TOP_K)], axis=1)
    whole = gather_rows(
        jnp.concatenate(
            [
                normed,
                keys_turned,
                tags.astype(jnp.bfloat16),
                jnp.zeros((tok_rows, LANES - QK_ROPE - 2 * TOP_K), jnp.bfloat16),
            ],
            axis=1,
        )
    )
    query_heads = queries[0].reshape(tok_rows, ATTENTION_HEADS, PLAIN_HEAD_WIDTH + QK_ROPE)
    query_turned = turn(
        query_heads[..., PLAIN_HEAD_WIDTH:].astype(jnp.float32),
        cos_local[:, None, :],
        sin_local[:, None, :],
    ).astype(jnp.bfloat16)
    query_full = jnp.concatenate(
        [
            query_heads[..., :PLAIN_HEAD_WIDTH],
            jnp.zeros((tok_rows, ATTENTION_HEADS, VALUE_HEAD_WIDTH), jnp.bfloat16),
            query_turned,
            jnp.zeros((tok_rows, ATTENTION_HEADS, LANES - QK_ROPE), jnp.bfloat16),
        ],
        axis=-1,
    )
    attended = attend(
        jnp.moveaxis(query_full, 1, 0), whole, latent_up_weight, start.reshape(1).astype(jnp.int32)
    )
    attn_normed = rms_scaled(attended, attn_gain).astype(jnp.bfloat16)
    mixed = jnp.dot(attn_normed, out_proj, preferred_element_type=jnp.float32)
    first = layer_norm(
        ALPHA * hidden_in[0].astype(jnp.float32) + mixed, norm1_gain, norm1_bias
    ).astype(jnp.bfloat16)
    slot_ids = jnp.arange(group * capacity, dtype=jnp.int32)
    inner = inner_of(lax.axis_size("sp"))
    plane = inner * lax.axis_size("dp")
    room = -(-capacity // 8) * 8
    far, near = lax.axis_index("sp") // inner, lax.axis_index("sp") % inner
    tag_from = key_value_latent.shape[2] + QK_ROPE
    line_tags = lax.dynamic_index_in_dim(
        whole[:, tag_from : tag_from + 2 * TOP_K].reshape(-1, inner, tok_rows, 2 * TOP_K),
        near, axis=1, keepdims=False,
    ).astype(jnp.int32)
    line_rows = (line_tags[..., :TOP_K] - far * plane) * room + line_tags[..., TOP_K:]
    row_ids = jnp.arange(plane * room, dtype=jnp.int32)
    picks = jnp.any(
        line_rows[:, None, :, :] == row_ids[None, :, None, None], axis=-1
    ).astype(jnp.bfloat16)
    arrived = dispatch_rows(first, picks, room)[:, :, :capacity]
    flat_rows = arrived.reshape(group * capacity, D)
    produced = (
        swiglu_rows(flat_rows, gate_proj[0], up_proj[0], down_proj[0])
        .astype(jnp.bfloat16)
        .reshape(group, capacity, D)
    )
    returned = lax.all_to_all(produced, ("sp", "dp"), split_axis=0, concat_axis=0, tiled=True)
    returned_flat = returned.reshape(group * capacity, D)
    weights = route_weights[0]
    gates = weights / jnp.sum(weights, axis=-1, keepdims=True) * ROUTED
    routed = jnp.zeros((tok_rows, D), jnp.float32)
    for column in range(TOP_K):
        picker = (places[:, column : column + 1] == slot_ids[None, :]).astype(jnp.bfloat16)
        picked = jnp.dot(picker, returned_flat, preferred_element_type=jnp.float32)
        routed = routed + gates[:, column : column + 1] * picked
    feed = routed + swiglu_rows(first, shared_gate, shared_up, shared_down)
    result = layer_norm(ALPHA * first.astype(jnp.float32) + feed, norm2_gain, norm2_bias).astype(
        jnp.bfloat16
    )
    return result.reshape(1, tok_rows, D)


def solution(mesh):
    in_specs = (
        P("dp", "sp", None),
        P("dp", "sp", None),
        P("dp", "sp", None),
        P("dp", "sp", None),
        P(),
        P(),
        P(),
        P(),
        P(),
        P(),
        P("dp", "sp", None),
        P("dp", "sp", None),
        P(("sp", "dp"), None, None),
        P(("sp", "dp"), None, None),
        P(("sp", "dp"), None, None),
        P(),
        P(),
        P(),
        P(),
        P(),
    )
    out_specs = P("dp", "sp", None)
    return jax.shard_map(
        per_device, mesh=mesh, in_specs=in_specs, out_specs=out_specs, check_vma=False
    )
```
